32 devices in a mesh: grp: 2 (over y), sp: 4 (over z), tp: 4 (over x, core).
Axes of the slice: x: 2, y: 2, z: 4, core: 2. Of those that a mesh axis runs over, the one named last changes fastest.
Arguments:
- tokens: bfloat16 [2048, 2048], P(('grp', 'sp', 'tp')), parts along dimension 0, may hold values from -6 to 6
- norm_gain: float32 [2048], replicated, may hold values from 0.1 to 1.9
- conv_b_w: bfloat16 [2048, 1024], P('sp', 'tp'), may hold values from -0.125 to 0.125
- conv_c_w: bfloat16 [2048, 1024], P('sp', 'tp'), may hold values from -0.125 to 0.125
- conv_x_w: bfloat16 [2048, 1024], P('sp', 'tp'), may hold values from -0.125 to 0.125
- query_w: bfloat16 [2048, 1024], P('sp', 'tp'), may hold values from -1 to 1
- key_w: bfloat16 [2048, 256], P('sp', 'tp'), may hold values from -2 to 2
- value_w: bfloat16 [2048, 256], P('sp', 'tp'), may hold values from -0.125 to 0.125
- conv_taps: float32 [3, 1024], P(None, 'tp'), may hold values from -3.5 to 3.5
- gate_cache: float32 [2048, 16], P('grp', 'tp'), parts along dimension 0, as said below
- out_conv_w: bfloat16 [1024, 2048], P('tp'), may hold values from -0.1875 to 0.1875
- out_attn_w: bfloat16 [1024, 2048], P('tp'), may hold values from -0.75 to 0.75
Outputs:
- mixed: bfloat16 [2048, 2048], P(('grp', 'sp', 'tp')), parts along dimension 0
- log_total: float32 [2048, 16], P(('grp', 'sp'), 'tp'), parts along dimension 0
The draws below stay inside these ranges and needn't reach their ends.
There are 2 independent parts, one for each index of `grp`. The reference program is written for one: setup_inputs(seed, part) draws one part's arguments, and reference() takes and returns one part's arrays. A program takes and returns all parts, laid end to end along the dimension named above; an argument that names none is the same for every part. Nothing has to cross between parts.
Inputs may be any that keep to these rules, and one draw needn't show every extreme that they name: `gate_cache`: never rises along positions; starts at or below zero.
All inputs are finite; a program needn't handle non-finite values.
Results may differ from the reference program's by a relative error of at most 0.017.
The reference program's roundings to bfloat16 on the way count: a program that leaves them out, or rounds other values in their place, can miss the bound.
Values may be sent and summed in bfloat16 or wider, within the bound.
A program may use at most 64 MiB of HBM per device.

```python
import jax
import jax.numpy as jnp
from jax import lax

D = 2048
CONV = 1024
QH = 16
KVH = 4
HD = 64
CW = 3
TOK_DEV = 256
SEQUENCE_LENGTH = 1024
N_TP = 4


def query_key_pair(key):
    base = jax.random.fold_in(key, 11)
    first, second = jax.random.split(base)
    query_f = jnp.clip(jax.random.normal(first, (D, QH * HD), jnp.float32), -5.0, 5.0) * D ** (-0.5)
    noise = jnp.clip(jax.random.normal(second, (D, KVH * HD), jnp.float32), -5.0, 5.0) * D ** (-0.5)
    key_f = noise
    return (query_f, jnp.clip(key_f, -2.0, 2.0))


def draw_query_w(key, part):
    pair = query_key_pair(key)
    return pair[0].astype(jnp.bfloat16)


def draw_key_w(key, part):
    pair = query_key_pair(key)
    return pair[1].astype(jnp.bfloat16)


def draw_gate_cache(key, part):
    keys = jax.random.split(key, 7)
    order = jax.random.permutation(keys[0], QH)
    fast = order < QH // 2
    fast_rate = 1.0 / 40.0 * jnp.exp(jax.random.uniform(keys[1], (QH,), jnp.float32, -0.5, 0.5))
    slow_rate = 0.6 / SEQUENCE_LENGTH * jnp.exp(jax.random.uniform(keys[6], (QH,), jnp.float32, -0.5, 0.5))
    decay_speed = jnp.where(fast, fast_rate, slow_rate)
    blocks = SEQUENCE_LENGTH // TOK_DEV
    scale_per_block = jnp.exp(jax.random.uniform(keys[2], (blocks, QH), jnp.float32, -0.9, 0.9))
    scale_per_block = jnp.repeat(scale_per_block, TOK_DEV, axis=0)
    coarse_estimate = jnp.exp(jax.random.uniform(keys[3], (SEQUENCE_LENGTH, QH), jnp.float32, -1.0, 1.0))
    chosen_locations = jax.random.randint(keys[4], (3,), 0, SEQUENCE_LENGTH)
    spike_amplitude = jnp.zeros((SEQUENCE_LENGTH,), jnp.float32).at[chosen_locations].set(1.0)
    objective_value = jax.random.uniform(keys[5], (QH,), jnp.float32, 0.2, 0.5) * (1.0 - fast.astype(jnp.float32))
    gate_logarithm = -(decay_speed[None, :] * scale_per_block * coarse_estimate + spike_amplitude[:, None] * objective_value[None, :])
    return jnp.cumsum(gate_logarithm, axis=0)


def levels(stream_key, extent, cuts, low, largest):
    loudness, own = 1.0, jax.random.fold_in(stream_key, 6)
    for dim, parts in cuts:
        steps = jnp.exp(jax.random.uniform(jax.random.fold_in(own, dim), (parts,), jnp.float32, low / len(cuts), largest / len(cuts)))
        loudness = loudness * jnp.repeat(steps, extent[dim] // parts).reshape([-1 if axis == dim else 1 for axis in range(len(extent))])
    return loudness


def bell_draw(key, dims, deviation, most, cuts=(), held_as=jnp.bfloat16):
    gain = levels(key, dims, cuts, -0.22, 0.18) if cuts else 1.0
    values = jax.random.normal(key, dims, jnp.float32) * deviation * gain
    return jnp.minimum(jnp.maximum(values, -most), most).astype(held_as)


def setup_inputs(seed: int = 0, part: int = 0) -> dict:
    seeds = jax.random.split(jax.random.key(seed), 13)
    part_splits = jax.random.split(jax.random.fold_in(seeds[12], part), 13)
    return {
        "tokens": bell_draw(part_splits[0], (SEQUENCE_LENGTH, D), 1.0, 6.0, ((0, 16),)),
        "norm_gain": jnp.clip(1.0 + 0.18 * jax.random.normal(seeds[1], (D,), jnp.float32), 0.1, 1.9),
        "conv_b_w": bell_draw(seeds[2], (D, CONV), D ** -0.5, 0.125, ((0, 4), (1, 4))),
        "conv_c_w": bell_draw(seeds[3], (D, CONV), D ** -0.5, 0.125, ((0, 4), (1, 4))),
        "conv_x_w": bell_draw(seeds[4], (D, CONV), D ** -0.5, 0.125, ((0, 4), (1, 4))),
        "query_w": draw_query_w(jax.random.fold_in(seeds[12], 71), part),
        "key_w": draw_key_w(jax.random.fold_in(seeds[12], 71), part),
        "value_w": bell_draw(seeds[7], (D, KVH * HD), D ** -0.5, 0.125, ((0, 4), (1, 4))),
        "conv_taps": bell_draw(seeds[8], (CW, CONV), CW ** -0.5, 3.5, ((1, 4),), jnp.float32),
        "gate_cache": draw_gate_cache(jax.random.fold_in(jax.random.fold_in(seeds[12], part), 71), part),
        "out_conv_w": bell_draw(seeds[10], (CONV, D), CONV ** -0.5, 0.1875, ((0, 4),)),
        "out_attn_w": bell_draw(seeds[11], (QH * HD, D), (QH * HD // 16) ** -0.5, 0.75, ((0, 4),)),
    }


def reference(tokens, norm_gain, conv_b_w, conv_c_w, conv_x_w, query_w, key_w, value_w, conv_taps, gate_cache, out_conv_w, out_attn_w):
    xf = tokens.astype(jnp.float32)
    scale_rows = lax.rsqrt(lax.optimization_barrier(jnp.mean(xf * xf, axis=-1, keepdims=True)) + 1e-05)
    normed = (xf * norm_gain).astype(jnp.bfloat16)

    def project(weight):
        return (jnp.dot(normed, weight, preferred_element_type=jnp.float32) * scale_rows).astype(jnp.bfloat16)
    gate_b = project(conv_b_w)
    gate_c = project(conv_c_w)
    conv_in = project(conv_x_w)
    query = project(query_w)
    key = project(key_w)
    value = project(value_w)
    conv_src = (gate_c.astype(jnp.float32) * conv_in.astype(jnp.float32)).astype(jnp.bfloat16)
    padded = jnp.concatenate([jnp.zeros((CW - 1, CONV), jnp.bfloat16), conv_src], axis=0)
    filtered = jnp.zeros((SEQUENCE_LENGTH, CONV), jnp.float32)
    for tap in range(CW):
        filtered = filtered + conv_taps[tap][None, :] * padded[tap:tap + SEQUENCE_LENGTH].astype(jnp.float32)
    conv_out = (gate_b.astype(jnp.float32) * filtered).astype(jnp.bfloat16)
    group = QH // KVH
    q_block = min(256, SEQUENCE_LENGTH)
    n_blocks = SEQUENCE_LENGTH // q_block
    heads_q = query.reshape(SEQUENCE_LENGTH, KVH, group, HD)
    keys_f = key.reshape(SEQUENCE_LENGTH, KVH, HD).astype(jnp.float32)
    values_f = value.reshape(SEQUENCE_LENGTH, KVH, HD).astype(jnp.float32)
    key_gate = gate_cache.T.reshape(KVH, group, 1, SEQUENCE_LENGTH)
    key_pos = jnp.arange(SEQUENCE_LENGTH, dtype=jnp.int32)

    def attend(index):
        begin = (index * q_block).astype(jnp.int32)
        q_rows = lax.dynamic_slice_in_dim(heads_q, begin, q_block, 0).astype(jnp.float32)
        q_gate = lax.dynamic_slice_in_dim(gate_cache, begin, q_block, 0)
        score = jnp.einsum('qgjd,kgd->gjqk', q_rows, keys_f) * HD ** (-0.5)
        score = score + q_gate.T.reshape(KVH, group, q_block, 1) - key_gate
        q_pos = begin + jnp.arange(q_block, dtype=jnp.int32)
        mask = key_pos[None, :] <= q_pos[:, None]
        score = jnp.where(mask, score, -1e+30)
        row_max = lax.optimization_barrier(jnp.max(score, axis=-1))
        weight = jnp.where(mask, jnp.exp(score - row_max[..., None]), 0.0)
        row_sum = lax.optimization_barrier(jnp.sum(weight, axis=-1))
        weight_bf = lax.optimization_barrier(weight.astype(jnp.bfloat16)).astype(jnp.float32)
        summed = jnp.einsum('gjqk,kgd->gjqd', weight_bf, values_f) / row_sum[..., None]
        out = summed.transpose(2, 0, 1, 3).reshape(q_block, QH * HD).astype(jnp.bfloat16)
        lse = (row_max + jnp.log(row_sum)).transpose(2, 0, 1).reshape(q_block, QH)
        return (out, lse)
    outs, lses = lax.map(attend, jnp.arange(n_blocks, dtype=jnp.int32))
    attn_out = outs.reshape(SEQUENCE_LENGTH, QH * HD)
    log_total = lses.reshape(SEQUENCE_LENGTH, QH)
    conv_part = CONV // N_TP
    attn_part = QH * HD // N_TP
    mixed = jnp.zeros((SEQUENCE_LENGTH, D), jnp.float32)
    for part in range(N_TP):
        term = jnp.dot(conv_out[:, part * conv_part:(part + 1) * conv_part], out_conv_w[part * conv_part:(part + 1) * conv_part], preferred_element_type=jnp.float32)
        term = term + jnp.dot(attn_out[:, part * attn_part:(part + 1) * attn_part], out_attn_w[part * attn_part:(part + 1) * attn_part], preferred_element_type=jnp.float32)
        mixed = mixed + term.astype(jnp.bfloat16).astype(jnp.float32)
    return (mixed.astype(jnp.bfloat16), log_total)
```

```python
import functools

import jax
import jax.numpy as jnp
from jax import lax
from jax.experimental import pallas as pl
from jax.experimental.pallas import tpu as pltpu
from jax.sharding import PartitionSpec as P

HD = 64
LANES = 128
MESH = pl.DeviceIdType.MESH
F32 = jnp.float32
BF16 = jnp.bfloat16


def layer_kernel(
    n_sp,
    n_tp,
    tokens_hbm,
    gain_hbm,
    wb_hbm,
    wc_hbm,
    wx_hbm,
    wq_hbm,
    wk_hbm,
    wv_hbm,
    taps_hbm,
    gate_hbm,
    oconv_hbm,
    oattn_hbm,
    mixed_ref,
    lse_ref,
    tok,
    normed,
    scale,
    gain,
    taps_own,
    taps_sib,
    gate_own,
    gate_sib,
    wb_ref,
    wc_ref,
    wx_ref,
    wq_ref,
    kv_ref,
    bc_all,
    x_all,
    q_all,
    kv_all,
    gates,
    pack,
    attn_o,
    conv_o,
    comb,
    lse_out,
    lse_in,
    wout,
    part,
    sib,
    fwd,
    xin,
    send_sem,
    tok_sem,
    w_sem,
    small_sem,
    kv_sem,
    out_sem,
    sum_sem,
    local_sem,
):
    g = lax.axis_index("grp")
    s = lax.axis_index("sp")
    t = lax.axis_index("tp")
    core = lax.rem(t, 2)
    first = t - core
    parity = lax.rem(s, 2)
    owner = core == parity
    across = {"grp": 1 - g}
    sibling = first + 1 - core
    far = lax.rem(t + 2, n_tp)
    far_sibling = lax.rem(sibling + 2, n_tp)
    z_near = s + 1 - 2 * parity
    z_two = lax.rem(s + 2, n_sp)
    z_three = n_sp - 1 - s
    late = s >= 2
    rows_own, width = tokens_hbm.shape
    depth = wb_hbm.shape[0]
    half = depth // 2
    count = rows_own * n_tp
    mine = 2 * count
    sub = rows_own // 2
    ch = wb_hbm.shape[1] // 2

    def block(index, size):
        return pl.ds(pl.multiple_of(index * size, size), size)

    barrier = pltpu.get_barrier_semaphore()
    for by in range(1, n_sp):
        for to in (t, sibling):
            pl.semaphore_signal(
                barrier,
                inc=1,
                device_id={"sp": lax.rem(s + by, n_sp), "tp": to},
                device_id_type=MESH,
            )
    for to in (sibling, far):
        pl.semaphore_signal(barrier, inc=1, device_id={"tp": to}, device_id_type=MESH)
    pl.semaphore_signal(barrier, inc=1, device_id=across, device_id_type=MESH)

    def tok_rows(z, x):
        return pl.ds(pl.multiple_of(HALO + z * count + x * rows_own, 16), rows_own)

    def tok_block(z, x):
        return tok.at[tok_rows(z, x)]

    pairs = (
        (tokens_hbm, tok_block(parity, t)),
        (wq_hbm, wq_ref),
        (wk_hbm, kv_ref.at[0]),
        (wv_hbm, kv_ref.at[1]),
        (wb_hbm, wb_ref),
        (wc_hbm, wc_ref),
        (wx_hbm, wx_ref),
        (gate_hbm, gate_own),
        (taps_hbm, taps_own),
        (gain_hbm, gain),
        (oconv_hbm, wout.at[pl.ds(0, 2 * ch)]),
        (oattn_hbm, wout.at[pl.ds(2 * ch, 2 * ch)]),
    )
    loads = [
        pltpu.make_async_copy(src, dst, local_sem.at[k]) for k, (src, dst) in enumerate(pairs)
    ]
    for copy in loads:
        copy.start()

    @pl.when(jnp.logical_not(late))
    def _():
        tok[:HALO, :] = jnp.zeros((HALO, width), BF16)
        pack[0, :, :, :] = jnp.zeros(pack.shape[1:], BF16)

    pl.semaphore_wait(barrier, 2 * n_sp + 1)

    used = [0]
    sent = []

    def send(src, dst, arrival, device, when=None):
        index = used[0]
        used[0] += 1
        copy = pltpu.make_async_remote_copy(
            src_ref=src,
            dst_ref=dst,
            send_sem=send_sem.at[index],
            recv_sem=arrival,
            device_id=device,
            device_id_type=MESH,
        )
        sent.append((copy, when))
        if when is None:
            copy.start()
        else:
            pl.when(when)(copy.start)
        return copy

    def arrived(ref, arrival):
        pltpu.make_async_remote_copy(
            src_ref=ref,
            dst_ref=ref,
            send_sem=send_sem.at[0],
            recv_sem=arrival,
            device_id=across,
            device_id_type=MESH,
        ).wait_recv()

    def tok_send(z, x, devices):
        here = tok_block(z, x)
        for device in devices:
            send(here, here, tok_sem.at[z * n_tp + x], device)

    def tok_wait(z, x):
        arrived(tok_block(z, x), tok_sem.at[z * n_tp + x])

    halo_sem = tok_sem.at[2 * n_tp]
    halo = tok.at[pl.ds(0, HALO)]

    MATS = {"q": 0, "kv": 1, "b": 2, "c": 3, "x": 4}
    lanes = {"q": (q_all, 0), "b": (bc_all, 0), "c": (bc_all, 1), "x": (x_all, 0)}
    local = {"q": wq_ref, "b": wb_ref, "c": wc_ref, "x": wx_ref}

    def w_place(m, z, start, size):
        if m == "kv":
            return kv_all.at[z, :, pl.ds(pl.multiple_of(start, half), size)]
        ref, k = lanes[m]
        rows = pl.ds(pl.multiple_of(z * depth + start, half), size)
        return ref.at[rows, pl.ds(k * ch, ch)]

    def w_source(m, to, start, size):
        if m == "kv":
            return kv_ref.at[to, :, pl.ds(pl.multiple_of(start, half), size)]
        cols = pl.ds(pl.multiple_of(to * ch, ch), ch)
        return local[m].at[pl.ds(pl.multiple_of(start, half), size), cols]

    def w_arrival(m, z, part_of):
        return w_sem.at[MATS[m] * 2 * n_sp + 2 * z + part_of]

    def w_send_far(mats):
        z = jnp.where(owner, z_two, z_three)
        for m in mats:
            for to in range(2):
                send(
                    w_source(m, to, g * half, half),
                    w_place(m, s, g * half, half),
                    w_arrival(m, s, g),
                    {"sp": z, "tp": first + to},
                )

    def w_send_near(mats):
        for m in mats:
            for to in range(2):
                send(
                    w_source(m, to, g * half, half),
                    w_place(m, s, g * half, half),
                    w_arrival(m, s, g),
                    {"sp": z_near, "tp": first + to},
                    jnp.logical_not(owner),
                )

    def w_send_here(mats):
        for m in mats:
            send(
                w_source(m, 1 - core, 0, depth),
                w_place(m, s, 0, depth),
                w_arrival(m, s, 0),
                {"tp": sibling},
                owner,
            )

            @pl.when(owner)
            def _(m=m):
                if m == "kv":
                    kv_all[s, :, :] = kv_ref[core]
                else:
                    ref, k = lanes[m]
                    own = local[m][...]
                    ref[block(s, depth), k * ch : (k + 1) * ch] = jnp.where(
                        core == 0, own[:, :ch], own[:, ch:]
                    )

    def w_over(mats, z):
        for m in mats:
            place = w_place(m, z, g * half, half)
            arrived(place, w_arrival(m, z, g))
            send(place, place, w_arrival(m, z, g), across)

    def w_here(mats):
        for m in mats:

            @pl.when(jnp.logical_not(owner))
            def _(m=m):
                arrived(w_place(m, s, 0, depth), w_arrival(m, s, 0))

    def w_across(mats, z):
        for m in mats:
            arrived(w_place(m, z, (1 - g) * half, half), w_arrival(m, z, 1 - g))

    others = (z_two, z_three, z_near)

    loads[0].wait()
    tok_send(parity, t, ({"sp": z_near}, {"tp": far}, {"tp": sibling}))
    tail_rows = pl.ds(pl.multiple_of(HALO + parity * count + (t + 1) * rows_own - HALO, 16), HALO)
    end = t == n_tp - 1
    send(tok.at[tail_rows], halo, halo_sem, {"sp": 2}, jnp.logical_and(s == 1, end))
    for copy in loads[1:4]:
        copy.wait()
    w_send_far(("q", "kv"))
    w_send_near(("q", "kv"))
    w_send_here(("q", "kv"))
    for copy in loads[4:7]:
        copy.wait()
    w_send_far(("b", "c"))
    w_send_near(("b", "c"))
    for copy in loads[7:10]:
        copy.wait()
    send(gate_own, gate_sib, small_sem.at[0], {"tp": sibling})
    send(taps_own, taps_sib, small_sem.at[1], {"tp": sibling})
    w_send_here(("b", "c", "x"))

    tok_wait(1 - parity, t)
    tok_send(1 - parity, t, ({"tp": far}, {"tp": sibling}))
    tok_wait(parity, far)
    tok_send(parity, far, ({"tp": sibling},))

    late_end = jnp.logical_and(late, end)

    @pl.when(late_end)
    def _():
        arrived(halo, halo_sem)

    send(halo, halo, halo_sem, {"sp": n_sp - 1}, jnp.logical_and(s == 2, end))
    send(halo, halo, halo_sem, {"tp": far}, late_end)
    send(halo, halo, halo_sem, {"tp": sibling}, late_end)
    for z in others:
        w_over(("q", "kv"), z)
    tok_wait(1 - parity, far)
    tok_send(1 - parity, far, ({"tp": sibling},))

    late_rest = jnp.logical_and(late, jnp.logical_not(end))

    @pl.when(late_rest)
    def _():
        arrived(halo, halo_sem)

    send(halo, halo, halo_sem, {"tp": sibling}, jnp.logical_and(late, t == 1))
    for x in (sibling, far_sibling):
        for z in (parity, 1 - parity):
            tok_wait(z, x)

    def normalize(rows, size):
        xf = tok[rows, :].astype(F32)
        square = jnp.sum(xf * xf, axis=-1, keepdims=True)
        normed[rows, :] = (xf * gain[...]).astype(BF16)
        scale[rows, :] = jnp.broadcast_to(
            lax.rsqrt(square / width + 1e-05), (size, scale.shape[1])
        )

    def normalize_block(i, unused):
        normalize(pl.ds(pl.multiple_of(HALO + i * rows_own, 16), rows_own), rows_own)
        return unused

    normalize(pl.ds(0, HALO), HALO)
    lax.fori_loop(0, 2 * n_tp, normalize_block, 0)

    w_here(("q", "kv"))
    for z in others:
        w_across(("q", "kv"), z)
    body = normed[HALO:, :]
    scale_body = scale[HALO:, :]
    query = jnp.dot(body, q_all[...], preferred_element_type=F32)
    query = (query * scale_body).astype(BF16) * BF16(HD**-0.5)
    keyed = jnp.zeros((mine, HD), F32)
    for z in range(n_sp):
        keyed = keyed + lax.dot_general(
            body[:, z * depth : (z + 1) * depth],
            kv_all[z],
            (((1,), (1,)), ((), ())),
            preferred_element_type=F32,
        )
    keyed = (keyed * scale_body[:, :HD]).astype(BF16)
    pack[1, core, :, :] = jnp.concatenate([keyed[:count], keyed[count:]], axis=1)
    early = jnp.logical_not(late)
    for to in range(2):
        send(
            pack.at[1, core],
            pack.at[0, core],
            kv_sem.at[core],
            {"sp": z_two, "tp": first + to},
            early,
        )
    send(pack.at[1, core], pack.at[1, core], kv_sem.at[2 + core], {"tp": sibling})
    w_send_far(("x",))
    w_send_near(("x",))

    for z in others:
        w_over(("b", "c"), z)
    w_here(("b", "c"))
    for z in others:
        w_across(("b", "c"), z)
    both = jnp.dot(normed[...], bc_all[...], preferred_element_type=F32)
    gates[...] = (both * jnp.concatenate([scale[...], scale[...]], axis=1)).astype(BF16)

    arrived(pack.at[1, 1 - core], kv_sem.at[3 - core])
    for k in range(2):

        @pl.when(late)
        def _(k=k):
            arrived(pack.at[0, k], kv_sem.at[k])

    for k, (own, other) in enumerate(((gate_own, gate_sib), (taps_own, taps_sib))):
        arrived(other, small_sem.at[k])
    gate_all = jnp.where(owner, gate_own[...], gate_sib[...])
    gate_two = jnp.where(core == 0, gate_all[:2], gate_all[2:])
    gate_here = jnp.where(late, gate_two[:, mine:], gate_two[:, :mine])
    gate_keys = jnp.concatenate([gate_two[:, :mine], gate_here], axis=1)
    taps_all = jnp.where(owner, taps_own[...], taps_sib[...])
    taps_here = jnp.where(core == 0, taps_all[:, :ch], taps_all[:, ch:])

    def unpacked(k):
        return jnp.concatenate(
            [pack[0, k, :, :HD], pack[0, k, :, HD:], pack[1, k, :, :HD], pack[1, k, :, HD:]],
            axis=0,
        )

    keys, values = unpacked(0), unpacked(1)

    def deliver(kind, out_ref, d, out):
        here = jnp.logical_and(parity == d, owner)
        device = {"sp": jnp.where(parity == d, s, z_near), "tp": first + parity}
        for r in range(2):
            for k in range(n_tp):
                start = k * rows_own + r * sub
                out_ref[r, d, k * sub : (k + 1) * sub] = out[start : start + sub]
            send(
                out_ref.at[r, d],
                comb.at[kind, r, core],
                out_sem.at[kind * 4 + r * 2 + core],
                device,
                jnp.logical_not(here),
            )

            @pl.when(here)
            def _(r=r):
                comb[kind, r, core] = out_ref[r, d]

    for d in (1, 0):
        rows = slice(d * count, (d + 1) * count)
        seen = mine + (d + 1) * count
        q_pos = mine + d * count + lax.broadcasted_iota(jnp.int32, (count, seen), 0)
        k_pos = lax.broadcasted_iota(jnp.int32, (count, seen), 1)
        visible = jnp.logical_and(k_pos <= q_pos, jnp.logical_or(late, k_pos >= mine))
        outs = []
        logs = []
        for j in range(2):
            score = lax.dot_general(
                query[rows, j * HD : (j + 1) * HD],
                keys[:seen],
                (((1,), (1,)), ((), ())),
                preferred_element_type=F32,
            )
            gate_row = gate_here[j : j + 1, rows]
            gate_column = jnp.broadcast_to(gate_row, (LANES, count)).T[:, :1]
            score = score + gate_column - gate_keys[j : j + 1, :seen]
            score = jnp.where(visible, score, -1e30)
            row_max = jnp.max(score, axis=-1, keepdims=True)
            weight = jnp.exp(score - row_max)
            row_sum = jnp.sum(weight, axis=-1, keepdims=True)
            out = jnp.dot(weight.astype(BF16), values[:seen], preferred_element_type=F32)
            outs.append((out / row_sum).astype(BF16))
            log = jnp.broadcast_to(row_max + jnp.log(row_sum), (count, LANES)).T
            logs.append(log[:1])
        deliver(0, attn_o, d, jnp.concatenate(outs, axis=1))
        lse_out[d, :2] = jnp.concatenate(logs, axis=0)
        here = jnp.logical_and(parity == d, owner)
        send(
            lse_out.at[d],
            lse_in.at[core],
            out_sem.at[8 + core],
            {"sp": jnp.where(parity == d, s, z_near), "tp": first + parity},
            jnp.logical_not(here),
        )

        @pl.when(here)
        def _(d=d):
            lse_in[core] = lse_out[d]

    for z in others:
        w_over(("x",), z)
    w_here(("x",))
    for z in others:
        w_across(("x",), z)
    conv_in = jnp.dot(normed[...], x_all[...], preferred_element_type=F32)
    conv_in = (conv_in * scale[...]).astype(BF16).astype(F32)
    conv_src = (gates[:, ch:].astype(F32) * conv_in).astype(BF16).astype(F32)
    taps = taps_hbm.shape[0]
    filtered = jnp.zeros((mine, ch), F32)
    for tap in range(taps):
        back = taps - 1 - tap
        moved = pltpu.roll(conv_src, back, axis=0) if back else conv_src
        filtered = filtered + taps_here[tap : tap + 1] * moved[HALO:]
    conv_out = (gates[HALO:, :ch].astype(F32) * filtered).astype(BF16)
    for d in (1, 0):
        deliver(1, conv_o, d, conv_out[d * count : (d + 1) * count])

    for copy in loads[10:]:
        copy.wait()

    chunks = 2
    wide = width // chunks

    def relay(r, c):
        cols = pl.ds(c * wide, wide)
        base = 3 * (chunks * r + c)
        for k in range(2):
            arrived(sib.at[r, k, :, cols], sum_sem.at[base + k])
        pair = part[r, far, :, cols].astype(F32) + sib[r, 1, :, cols].astype(F32)
        fwd[r, :, cols] = pair.astype(BF16)
        send(fwd.at[r, :, cols], xin.at[r, :, cols], sum_sem.at[base + 2], {"tp": far})

    last = None
    for r in range(2):
        for kind in range(2):
            for k in range(2):

                @pl.when(jnp.logical_not(jnp.logical_and(owner, core == k)))
                def _(kind=kind, r=r, k=k):
                    arrived(comb.at[kind, r, k], out_sem.at[kind * 4 + r * 2 + k])

        gathered = jnp.concatenate(
            [comb[1, r, 0], comb[1, r, 1], comb[0, r, 0], comb[0, r, 1]], axis=1
        )
        for c in range(chunks):
            cols = pl.ds(c * wide, wide)
            term = jnp.dot(gathered, wout[:, cols], preferred_element_type=F32).astype(BF16)
            for k in range(n_tp):
                part[r, k, :, cols] = term[k * sub : (k + 1) * sub]
            for k, to in ((1, far_sibling), (0, sibling)):
                send(
                    part.at[r, to, :, cols],
                    sib.at[r, k, :, cols],
                    sum_sem.at[3 * (chunks * r + c) + k],
                    {"tp": sibling},
                )
            if last is not None:
                relay(*last)
            last = (r, c)
    relay(*last)
    for k in range(2):

        @pl.when(jnp.logical_not(jnp.logical_and(owner, core == k)))
        def _(k=k):
            arrived(lse_in.at[k], out_sem.at[8 + k])

        lse_ref[2 * k : 2 * k + 2, :] = lse_in[k, :2]
    for r in range(2):
        for c in range(chunks):
            cols = pl.ds(c * wide, wide)
            arrived(xin.at[r, :, cols], sum_sem.at[3 * (chunks * r + c) + 2])
            whole = part[r, t, :, cols].astype(F32) + sib[r, 0, :, cols].astype(F32)
            whole = whole + xin[r, :, cols].astype(F32)
            mixed_ref[r * sub : (r + 1) * sub, cols] = whole.astype(BF16)
    for copy, when in sent:
        if when is None:
            copy.wait_send()
        else:
            pl.when(when)(copy.wait_send)


COPIES = 192
HALO = 16


def in_one_kernel(
    n_sp,
    n_tp,
    tokens,
    norm_gain,
    conv_b_w,
    conv_c_w,
    conv_x_w,
    query_w,
    key_w,
    value_w,
    conv_taps,
    gate_cache,
    out_conv_w,
    out_attn_w,
):
    rows, width = tokens.shape
    count = rows * n_tp
    mine = 2 * count
    depth, channels = conv_b_w.shape
    ch = channels // 2
    heads = gate_cache.shape[1]
    vmem = pl.BlockSpec(memory_space=pltpu.VMEM)
    hbm = pl.BlockSpec(memory_space=pl.ANY)
    out_rows = out_conv_w.shape[0] + out_attn_w.shape[0]
    dma = pltpu.SemaphoreType.DMA
    gate_rows = gate_cache.T
    mixed, log_rows = pl.pallas_call(
        functools.partial(layer_kernel, n_sp, n_tp),
        out_shape=(
            jax.ShapeDtypeStruct((rows, width), BF16),
            jax.ShapeDtypeStruct((heads, count), F32),
        ),
        in_specs=[hbm] * 12,
        out_specs=(vmem, vmem),
        scratch_shapes=[
            pltpu.VMEM((HALO + mine, width), BF16),
            pltpu.VMEM((HALO + mine, width), BF16),
            pltpu.VMEM((HALO + mine, LANES), F32),
            pltpu.VMEM((1, width), F32),
            pltpu.VMEM(conv_taps.shape, F32),
            pltpu.VMEM(conv_taps.shape, F32),
            pltpu.VMEM(gate_rows.shape, F32),
            pltpu.VMEM(gate_rows.shape, F32),
            pltpu.VMEM(conv_b_w.shape, BF16),
            pltpu.VMEM(conv_c_w.shape, BF16),
            pltpu.VMEM(conv_x_w.shape, BF16),
            pltpu.VMEM(query_w.shape, BF16),
            pltpu.VMEM((2, key_w.shape[1], depth), BF16),
            pltpu.VMEM((width, 2 * ch), BF16),
            pltpu.VMEM((width, ch), BF16),
            pltpu.VMEM((width, ch), BF16),
            pltpu.VMEM((n_sp, key_w.shape[1], depth), BF16),
            pltpu.VMEM((HALO + mine, 2 * ch), BF16),
            pltpu.VMEM((2, 2, count, 2 * HD), BF16),
            pltpu.VMEM((2, 2, count // 2, ch), BF16),
            pltpu.VMEM((2, 2, count // 2, ch), BF16),
            pltpu.VMEM((2, 2, 2, count // 2, ch), BF16),
            pltpu.VMEM((2, 8, count), F32),
            pltpu.VMEM((2, 8, count), F32),
            pltpu.VMEM((out_rows, width), BF16),
            pltpu.VMEM((2, n_tp, rows // 2, width), BF16),
            pltpu.VMEM((2, 2, rows // 2, width), BF16),
            pltpu.VMEM((2, rows // 2, width), BF16),
            pltpu.VMEM((2, rows // 2, width), BF16),
            dma((COPIES,)),
            dma((2 * n_tp + 1,)),
            dma((5 * 2 * n_sp,)),
            dma((2,)),
            dma((4,)),
            dma((10,)),
            dma((12,)),
            dma((12,)),
        ],
        compiler_params=pltpu.CompilerParams(
            collective_id=0, has_side_effects=True, vmem_limit_bytes=60 * 1024 * 1024
        ),
    )(
        tokens,
        norm_gain.reshape(1, width),
        conv_b_w,
        conv_c_w,
        conv_x_w,
        query_w,
        key_w.T,
        value_w.T,
        conv_taps,
        gate_rows,
        out_conv_w,
        out_attn_w,
    )
    return mixed, log_rows.T


def passed_along(value, axis, by):
    count = lax.axis_size(axis)
    pairs = [(i, i + by) for i in range(count) if 0 <= i + by < count]
    return lax.ppermute(value, axis, pairs)


def on_device(
    tokens,
    norm_gain,
    conv_b_w,
    conv_c_w,
    conv_x_w,
    query_w,
    key_w,
    value_w,
    conv_taps,
    gate_cache,
    out_conv_w,
    out_attn_w,
):
    rows = lax.all_gather(tokens, "tp", axis=0, tiled=True)
    count = rows.shape[0]
    xf = rows.astype(jnp.float32)
    scale_rows = lax.rsqrt(jnp.mean(xf * xf, axis=-1, keepdims=True) + 1e-05)
    normed = (xf * norm_gain).astype(jnp.bfloat16)

    def contract_all(pieces):
        width = pieces[0].shape[0]
        return tuple(
            (jnp.dot(normed, piece, preferred_element_type=jnp.float32) for piece in pieces)
        )

    conv_sums = contract_all(
        (
            lax.all_gather(conv_b_w, "sp", axis=0, tiled=True),
            lax.all_gather(conv_c_w, "sp", axis=0, tiled=True),
            lax.all_gather(conv_x_w, "sp", axis=0, tiled=True),
        )
    )
    attn_sums = contract_all(
        (
            lax.all_gather(query_w, "sp", axis=0, tiled=True),
            lax.all_gather(key_w, "sp", axis=0, tiled=True),
            lax.all_gather(value_w, "sp", axis=0, tiled=True),
        )
    )
    sums = conv_sums + attn_sums
    gate_b, gate_c, conv_in, query, key, value = [
        (total * scale_rows).astype(jnp.bfloat16) for total in sums
    ]
    taps = conv_taps.shape[0]
    channels = conv_in.shape[1]
    conv_src = (gate_c.astype(jnp.float32) * conv_in.astype(jnp.float32)).astype(jnp.bfloat16)
    earlier = passed_along(conv_src[count - (taps - 1) :], "sp", 1)
    padded = jnp.concatenate([earlier, conv_src], axis=0)
    filtered = jnp.zeros((count, channels), jnp.float32)
    for tap in range(taps):
        filtered = filtered + conv_taps[tap][None, :] * padded[tap : tap + count].astype(
            jnp.float32
        )
    conv_out = (gate_b.astype(jnp.float32) * filtered).astype(jnp.bfloat16)
    heads_dev = gate_cache.shape[1]
    kv_dev = key.shape[1] // HD
    group = heads_dev // kv_dev
    half = count // 2
    sp_index = lax.axis_index("sp")
    own_start = sp_index * count
    scale = HD ** (-0.5)
    later_query = query[half:]
    later_start = own_start + half

    def prepare(q_rows, begin):
        heads_q = q_rows.reshape(half, kv_dev, group, HD)
        q_gate = lax.dynamic_slice_in_dim(gate_cache, begin, half, 0).T.reshape(
            kv_dev, group, half, 1
        )
        q_pos = begin + jnp.arange(half, dtype=jnp.int32)
        return (heads_q, q_gate, q_pos)

    sides = (prepare(query[:half], own_start), prepare(later_query, later_start))

    def absorb(carry, side, key_rows, value_rows, begin):
        heads_q, q_gate, q_pos = side
        run_max, run_sum, acc = carry
        width = key_rows.shape[0]
        key_heads = key_rows.reshape(width, kv_dev, HD)
        value_heads = value_rows.reshape(width, kv_dev, HD)
        score = (
            jnp.einsum("qgjd,kgd->gjqk", heads_q, key_heads, preferred_element_type=jnp.float32)
            * scale
        )
        key_gate = lax.dynamic_slice_in_dim(gate_cache, begin, width, 0).T.reshape(
            kv_dev, group, 1, width
        )
        score = score + q_gate - key_gate
        mask = (begin + jnp.arange(width, dtype=jnp.int32))[None, :] <= q_pos[:, None]
        score = jnp.where(mask, score, -1e30)
        new_max = jnp.maximum(run_max, jnp.max(score, axis=-1))
        weight = jnp.where(mask, jnp.exp(score - new_max[..., None]), 0.0)
        factor = jnp.exp(run_max - new_max)
        new_sum = run_sum * factor + jnp.sum(weight, axis=-1)
        product = jnp.einsum(
            "gjqk,kgd->gjqd",
            weight.astype(jnp.bfloat16),
            value_heads,
            preferred_element_type=jnp.float32,
        )
        return (new_max, new_sum, acc * factor[..., None] + product)

    def guarded(carry, side, key_rows, value_rows, begin):

        def visit_rows(state):
            return absorb(state, side, key_rows, value_rows, begin)

        def keep(state):
            return state

        return lax.cond(begin <= side[2][half - 1], visit_rows, keep, carry)

    def absorb_both(carry, key_rows, value_rows, begin):
        return (
            guarded(carry[0], sides[0], key_rows, value_rows, begin),
            guarded(carry[1], sides[1], key_rows, value_rows, begin),
        )

    def fresh():
        return (
            jnp.full((kv_dev, group, half), -1e30, jnp.float32),
            jnp.zeros((kv_dev, group, half), jnp.float32),
            jnp.zeros((kv_dev, group, half, HD), jnp.float32),
        )

    key_rows = lax.all_gather(key, "sp", axis=0, tiled=True)
    value_rows = lax.all_gather(value, "sp", axis=0, tiled=True)
    width = key_rows.shape[0]
    step = 512
    key_blocks = key_rows.reshape(width // step, step, key_rows.shape[1])
    value_blocks = value_rows.reshape(width // step, step, value_rows.shape[1])
    firsts = step * jnp.arange(width // step, dtype=jnp.int32)

    def visit(state, inputs):
        return (absorb_both(state, inputs[0], inputs[1], inputs[2]), None)

    result, unused = lax.scan(visit, (fresh(), fresh()), (key_blocks, value_blocks, firsts))

    def finish(state):
        run_max, run_sum, acc = state
        out = (
            (acc / run_sum[..., None])
            .transpose(2, 0, 1, 3)
            .reshape(half, heads_dev * HD)
            .astype(jnp.bfloat16)
        )
        lse = (run_max + jnp.log(run_sum)).transpose(2, 0, 1).reshape(half, heads_dev)
        return (out, lse)

    early_out, early_lse = finish(result[0])
    later_out, later_lse = finish(result[1])
    attn_out = jnp.concatenate([early_out, later_out], axis=0)
    log_total = jnp.concatenate([early_lse, later_lse], axis=0)
    term = jnp.dot(conv_out, out_conv_w, preferred_element_type=jnp.float32)
    mixed = lax.psum_scatter(
        (term + jnp.dot(attn_out, out_attn_w, preferred_element_type=jnp.float32)).astype(
            jnp.bfloat16
        ),
        "tp",
        scatter_dimension=0,
        tiled=True,
    )
    return (mixed, log_total)


def solution(mesh):
    placed = (
        P(("grp", "sp", "tp"), None),
        P(),
        P("sp", "tp"),
        P("sp", "tp"),
        P("sp", "tp"),
        P("sp", "tp"),
        P("sp", "tp"),
        P("sp", "tp"),
        P(None, "tp"),
        P("grp", "tp"),
        P("tp", None),
        P("tp", None),
    )
    sizes = dict(mesh.shape)

    def on_one(*args):
        channels, key_width = args[2].shape[1], args[6].shape[1]
        grid = (sizes["grp"], sizes["sp"], sizes["tp"])
        fits = channels == 2 * LANES and args[5].shape[1] == channels and key_width == HD
        if grid == (2, 4, 4) and fits and args[9].shape[1] * HD == channels:
            return in_one_kernel(sizes["sp"], sizes["tp"], *args)
        return on_device(*args)

    return jax.shard_map(
        on_one,
        mesh=mesh,
        in_specs=placed,
        out_specs=(P(("grp", "sp", "tp"), None), P(("grp", "sp"), "tp")),
        check_vma=False,
    )
```
